32 devices in a mesh: sp: 8 (over z, y), tp: 4 (over x, core).
Axes of the slice: x: 2, y: 2, z: 4, core: 2. Of those that a mesh axis runs over, the one named last changes fastest.
Arguments:
- resid_in: bfloat16 [2048, 2048], P('sp'), may hold values from -6 to 6
- query_latent: bfloat16 [2048, 768], P('sp'), may hold values from -6 to 6
- kv_latent: bfloat16 [2048, 512], P('sp'), may hold values from -6 to 6
- rotary_key: bfloat16 [2048, 64], P('sp'), may hold values from -200 to 200
- query_gain: float32 [768], replicated, may hold values from 0.1 to 1.9
- kv_gain: float32 [512], replicated, may hold values from 0.1 to 1.9
- w_query_plain: bfloat16 [768, 2048], P(None, 'tp'), may hold values from -0.875 to 0.875
- w_query_rotary: bfloat16 [768, 1024], P(None, 'tp'), may hold values from -0.875 to 0.875
- w_key_plain: bfloat16 [512, 2048], P(None, 'tp'), may hold values from -0.25 to 0.25
- w_value: bfloat16 [512, 2048], P(None, 'tp'), may hold values from -0.25 to 0.25
- w_output: bfloat16 [2048, 2048], P('tp'), may hold values from -0.125 to 0.125
- ffn_gain: float32 [2048], replicated, may hold values from 0.1 to 1.9
- w_gate: bfloat16 [2048, 5632], P('sp', 'tp'), may hold values from -0.125 to 0.125
- w_up: bfloat16 [2048, 5632], P('sp', 'tp'), may hold values from -0.125 to 0.125
- w_down: bfloat16 [5632, 2048], P('tp', 'sp'), may hold values from -0.078125 to 0.078125
Outputs:
- resid_out: bfloat16 [2048, 2048], P(('sp', 'tp'))
The draws below stay inside these ranges and needn't reach their ends.
All inputs are finite; a program needn't handle non-finite values.
Results may differ from the reference program's by a relative error of at most 0.014.
The reference program's roundings to bfloat16 on the way count: a program that leaves them out, or rounds other values in their place, can miss the bound.
Values may be sent and summed in bfloat16 or wider, within the bound.
No kernel may reach another device: no remote copies, remote signals or barrier semaphores. Data moves between devices by JAX's collectives and lax.ppermute only.
A program may use at most 192 MiB of HBM per device.

```python
import jax
import jax.numpy as jnp
from jax import lax

D = 2048
HEADS = 16
QR = 768
KVR = 512
NOPE = 128
ROPE = 64
VDIM = 128
FF = 5632
TOK_DEV = 256
SEQ = 2048


def draw_rotary_key(key, part):
    first = jax.random.fold_in(jax.random.fold_in(key, 11), 0)
    base = jnp.clip(jax.random.normal(first, (SEQ, ROPE), jnp.float32), -5.0, 5.0)
    return base.astype(jnp.bfloat16)


def shard_levels(own_key, shape, cuts, smallest, top_value):
    factor_of = 1.0
    for dim, blocks in cuts:
        draws = jax.random.uniform(jax.random.fold_in(jax.random.fold_in(own_key, 6), dim), (blocks,), jnp.float32, smallest / len(cuts), top_value / len(cuts))
        factor_of = factor_of * jnp.repeat(jnp.exp(draws), shape[dim] // blocks).reshape((-1,) + (1,) * (len(shape) - 1 - dim))
    return factor_of


def normal_values(stream_key, dims, spread, most, cuts=(), kind=jnp.bfloat16):
    drawn = jax.random.normal(stream_key, dims, jnp.float32) * spread
    if len(cuts) > 0:
        drawn = shard_levels(stream_key, dims, cuts, -0.22, 0.18) * drawn
    return jnp.clip(drawn, min=-most, max=most).astype(kind)


def setup_inputs(seed: int = 0) -> dict:
    key_of = jax.random.split(jax.random.key(seed), 16)
    resid_in = normal_values(key_of[0], (SEQ, D), 1.0, 6.0, ((0, 8),))
    query_latent = normal_values(key_of[1], (SEQ, QR), 1.0, 6.0, ((0, 8),))
    kv_latent = normal_values(key_of[2], (SEQ, KVR), 1.0, 6.0, ((0, 8),))
    rotary_key = draw_rotary_key(jax.random.fold_in(key_of[15], 71), 0)
    query_gain = jnp.clip(1.0 + 0.18 * jax.random.normal(key_of[4], (QR,), jnp.float32), 0.1, 1.9)
    kv_gain = jnp.clip(1.0 + 0.18 * jax.random.normal(key_of[5], (KVR,), jnp.float32), 0.1, 1.9)
    w_query_plain = normal_values(key_of[6], (QR, HEADS * NOPE), (QR // 16) ** -0.5, 0.875, ((1, 4),))
    w_query_rotary = normal_values(key_of[7], (QR, HEADS * ROPE), (QR // 16) ** -0.5, 0.875, ((1, 4),))
    w_key_plain = normal_values(key_of[8], (KVR, HEADS * NOPE), KVR ** -0.5, 0.25, ((1, 4),))
    w_value = normal_values(key_of[9], (KVR, HEADS * VDIM), KVR ** -0.5, 0.25, ((1, 4),))
    w_output = normal_values(key_of[10], (HEADS * VDIM, D), (HEADS * VDIM) ** -0.5, 0.125, ((0, 4),))
    ffn_gain = jnp.clip(1.0 + 0.18 * jax.random.normal(key_of[11], (D,), jnp.float32), 0.1, 1.9)
    w_gate = normal_values(key_of[12], (D, FF), D ** -0.5, 0.125, ((0, 8), (1, 4)))
    w_up = normal_values(key_of[13], (D, FF), D ** -0.5, 0.125, ((0, 8), (1, 4)))
    w_down = normal_values(key_of[14], (FF, D), FF ** -0.5, 0.078125, ((0, 4), (1, 8)))
    return dict(resid_in=resid_in, query_latent=query_latent, kv_latent=kv_latent, rotary_key=rotary_key, query_gain=query_gain, kv_gain=kv_gain, w_query_plain=w_query_plain, w_query_rotary=w_query_rotary, w_key_plain=w_key_plain, w_value=w_value, w_output=w_output, ffn_gain=ffn_gain, w_gate=w_gate, w_up=w_up, w_down=w_down)


def normed(values, gain):
    wide = values.astype(jnp.float32)
    return wide * lax.rsqrt(lax.optimization_barrier(jnp.mean(wide * wide, axis=-1, keepdims=True)) + 1e-06) * gain.astype(jnp.float32)

def rotate(values, cosine, sine):
    half = values.shape[-1] // 2
    first = values[..., :half]
    second = values[..., half:]
    return jnp.concatenate([first * cosine - second * sine, second * cosine + first * sine], axis=-1)

def reference(resid_in, query_latent, kv_latent, rotary_key, query_gain, kv_gain, w_query_plain, w_query_rotary, w_key_plain, w_value, w_output, ffn_gain, w_gate, w_up, w_down):
    length = resid_in.shape[0]
    position = jnp.arange(length, dtype=jnp.float32)
    freq = 10000.0 ** (-jnp.arange(0, ROPE, 2, dtype=jnp.float32) / ROPE)
    angle = position[:, None] * freq[None, :]
    cosine = jnp.cos(angle)
    sine = jnp.sin(angle)
    q_norm = normed(query_latent, query_gain).astype(jnp.bfloat16)
    kv_norm = normed(kv_latent, kv_gain).astype(jnp.bfloat16)
    key_rot = rotate(rotary_key.astype(jnp.float32), cosine, sine).astype(jnp.bfloat16)
    q_plain = jnp.dot(q_norm, w_query_plain, preferred_element_type=jnp.float32).astype(jnp.bfloat16).reshape(length, HEADS, NOPE)
    q_raw = jnp.dot(q_norm, w_query_rotary, preferred_element_type=jnp.float32).reshape(length, HEADS, ROPE)
    q_rot = rotate(q_raw, cosine[:, None, :], sine[:, None, :]).astype(jnp.bfloat16)
    k_plain = jnp.dot(kv_norm, w_key_plain, preferred_element_type=jnp.float32).astype(jnp.bfloat16).reshape(length, HEADS, NOPE)
    values = jnp.dot(kv_norm, w_value, preferred_element_type=jnp.float32).astype(jnp.bfloat16).reshape(length, HEADS, VDIM)
    k_wide = k_plain.astype(jnp.float32)
    v_wide = values.astype(jnp.float32)
    r_wide = key_rot.astype(jnp.float32)
    scale = (NOPE + ROPE) ** (-0.5)
    blocks = length // TOK_DEV

    def attend(pair):
        q_a, q_b = pair
        score = (jnp.einsum('qhd,khd->hqk', q_a.astype(jnp.float32), k_wide) + jnp.einsum('qhr,kr->hqk', q_b.astype(jnp.float32), r_wide)) * scale
        top = lax.optimization_barrier(jnp.max(score, axis=-1, keepdims=True))
        weight = jnp.exp(score - top)
        total = lax.optimization_barrier(jnp.sum(weight, axis=-1))
        mixed = jnp.einsum('hqk,khd->qhd', weight.astype(jnp.bfloat16).astype(jnp.float32), v_wide)
        return (mixed / jnp.transpose(total)[:, :, None]).astype(jnp.bfloat16)
    attn = lax.map(attend, (q_plain.reshape(blocks, TOK_DEV, HEADS, NOPE), q_rot.reshape(blocks, TOK_DEV, HEADS, ROPE)))
    attn = attn.reshape(length, HEADS * VDIM)
    mid = resid_in.astype(jnp.float32) + jnp.dot(attn, w_output, preferred_element_type=jnp.float32)
    h_norm = normed(mid, ffn_gain).astype(jnp.bfloat16)
    gate = jnp.dot(h_norm, w_gate, preferred_element_type=jnp.float32)
    upper = jnp.dot(h_norm, w_up, preferred_element_type=jnp.float32)
    hidden = (jax.nn.silu(gate) * upper).astype(jnp.bfloat16)
    return (mid + jnp.dot(hidden, w_down, preferred_element_type=jnp.float32)).astype(jnp.bfloat16)
```

```python
import functools

import jax
import jax.numpy as jnp
from jax import lax
from jax.experimental import pallas as pl
from jax.experimental.pallas import tpu as pltpu
from jax.sharding import PartitionSpec as P

NOPE = 128
ROPE = 64
VDIM = 128
EPS = 1e-06


F32 = jnp.float32
BF16 = jnp.bfloat16
NT = (((1,), (1,)), ((), ()))
NN = (((1,), (0,)), ((), ()))


def mm(a, b, dims=NN):
    return lax.dot_general(a, b, dims, preferred_element_type=F32)


def normed(values, gain):
    wide = values.astype(F32)
    return wide * lax.rsqrt(jnp.mean(wide * wide, axis=-1, keepdims=True) + EPS) * gain


def attention_kernel(n, half, c_ref, qp_ref, qr_ref, wk_ref, wv_ref, wo_ref, *rest):
    pieces = rest[:n]
    own_ref, other_ref = rest[n : n + 2]
    k_ref, v_ref, r_ref, attn_ref = rest[n + 2 :]
    rows = r_ref.shape[0] * half // wk_ref.shape[0]
    width = wk_ref.shape[0]
    for i, piece in enumerate(pieces):
        lat = piece[:half, :]
        at = pl.ds(i * half, half)
        k_ref[at, :] = mm(lat, wk_ref[...]).astype(BF16)
        v_ref[at, :] = mm(lat, wv_ref[...]).astype(BF16)
        for b in range(width // half):
            r_ref[pl.ds(b * rows, rows), at] = piece[half : half + rows, b * half : (b + 1) * half]
    scale = (NOPE + ROPE) ** (-0.5)
    heads = wk_ref.shape[1] // NOPE
    for h in range(heads):
        lane = slice(h * NOPE, (h + 1) * NOPE)
        score = mm(qp_ref[:, lane], k_ref[:, lane], NT)
        score = (score + mm(qr_ref[:, h * ROPE : (h + 1) * ROPE], r_ref[...])) * scale
        top = jnp.max(score, axis=-1, keepdims=True)
        weight = jnp.exp(score - top)
        total = jnp.sum(weight, axis=-1, keepdims=True)
        mixed = mm(weight.astype(BF16), v_ref[:, lane])
        attn_ref[:, lane] = (mixed / total).astype(BF16)
    out = mm(attn_ref[...], wo_ref[...])
    c = c_ref[0]
    share = out.shape[0] // 4
    first = jnp.concatenate([out[:share], out[2 * share : 3 * share]], axis=0)
    second = jnp.concatenate([out[share : 2 * share], out[3 * share :]], axis=0)
    mine = c == 0
    own_ref[...] = jnp.where(mine, first, second)
    other_ref[...] = jnp.where(mine, second, first).astype(BF16)


def ffn_kernel(n_tok, n_blk, fcols, b_ref, *rest):
    tok = rest[:n_tok]
    first = rest[n_tok : n_tok + n_blk]
    second = rest[n_tok + n_blk : n_tok + 2 * n_blk]
    own_ref, other_ref, h_ref = rest[n_tok + 2 * n_blk :]
    share = tok[0].shape[0]
    for i, t in enumerate(tok):
        h_ref[i * share : (i + 1) * share, :] = t[...]
    width = first[0].shape[1]
    count = n_tok * share
    hid = []
    for group in (first, second):
        gate = jnp.zeros((count, fcols), F32)
        upper = jnp.zeros((count, fcols), F32)
        for i, w in enumerate(group):
            block = h_ref[:, pl.ds(pl.multiple_of(b_ref[i] * width, width), width)]
            gate = gate + mm(block, w[:fcols, :], NT)
            upper = upper + mm(block, w[fcols : 2 * fcols, :], NT)
        hid.append((gate * jax.nn.sigmoid(gate) * upper).astype(BF16))
    mid = count // 2
    for i in range(n_blk):
        at = pl.ds(pl.multiple_of(b_ref[i] * width, width), width)
        out = mm(hid[0], first[i][2 * fcols :, :]) + mm(hid[1], second[i][2 * fcols :, :])
        own_ref[:, at] = out[:mid]
        other_ref[:, at] = out[mid:].astype(BF16)


def vmem(n):
    return [pl.BlockSpec(memory_space=pltpu.VMEM)] * n


SMEM = pl.BlockSpec(memory_space=pltpu.SMEM)


def make(mesh):
    n_sp, n_tp = mesh.shape["sp"], mesh.shape["tp"]
    nz = 4
    ny = n_sp // nz
    nc = 2
    nx = n_tp // nc

    def permute(value, dz=0, dy=0, dx=0, dc=0):
        pairs = []
        for s in range(n_sp):
            for t in range(n_tp):
                z, y = divmod(s, ny)
                x, c = divmod(t, nc)
                s2 = (z + dz) % nz * ny + (y + dy) % ny
                t2 = (x + dx) % nx * nc + (c + dc) % nc
                pairs.append((s * n_tp + t, s2 * n_tp + t2))
        return lax.ppermute(value, ("sp", "tp"), pairs)

    def shards(
        resid_in,
        query_latent,
        kv_latent,
        rotary_key,
        query_gain,
        kv_gain,
        w_query_plain,
        w_query_rotary,
        w_key_plain,
        w_value,
        w_output,
        ffn_gain,
        w_gate,
        w_up,
        w_down,
    ):
        tok, width = resid_in.shape
        kvr = kv_latent.shape[1]
        heads = w_query_plain.shape[1] // NOPE
        s_id = lax.axis_index("sp")
        t_id = lax.axis_index("tp")
        z, y = s_id // ny, s_id % ny
        x, c = t_id // nc, t_id % nc
        position = (s_id * tok + jnp.arange(tok, dtype=jnp.int32)).astype(F32)
        freq = 10000.0 ** (-jnp.arange(0, ROPE, 2, dtype=F32) / ROPE)
        angle = position[:, None] * freq[None, :]
        cosine = jnp.cos(angle)
        sine = jnp.sin(angle)

        half = tok // nc
        lat = normed(lax.dynamic_slice_in_dim(kv_latent, c * half, half, 0), kv_gain).astype(BF16)
        key = lax.dynamic_slice_in_dim(rotary_key, c * half, half, 0).astype(F32)
        cos_k = lax.dynamic_slice_in_dim(cosine, c * half, half, 0)
        sin_k = lax.dynamic_slice_in_dim(sine, c * half, half, 0)
        ka, kb = key[:, : ROPE // 2], key[:, ROPE // 2 :]
        rot = jnp.concatenate([ka * cos_k - kb * sin_k, kb * cos_k + ka * sin_k], axis=1)
        rot = rot.astype(BF16).T
        per = kvr // half
        rows = ROPE // per
        rot = jnp.concatenate([rot[b * rows : (b + 1) * rows] for b in range(per)], axis=1)
        piece = jnp.concatenate([lat, rot], axis=0)
        kv = [piece] + [permute(piece, dz=i) for i in range(1, nz)]
        kv = kv + [permute(p, dy=j) for j in range(1, ny) for p in kv]
        kv = kv + [permute(p, dc=1) for p in kv]

        fcols = w_gate.shape[1] // nz
        wg = w_gate.T.reshape(nz, fcols, -1)
        wu = w_up.T.reshape(nz, fcols, -1)
        wd = w_down.reshape(nz, fcols, -1)
        packed = jnp.concatenate([wg, wu, wd], axis=1)

        def weights_for(i):
            return lax.dynamic_index_in_dim(packed, (z + i) % nz, 0, keepdims=False)

        base = [weights_for(0)] + [permute(weights_for(i), dz=i) for i in range(1, nz)]
        mine, theirs, blocks = [], [], []
        for i in range(nz):
            across = permute(base[i], dx=1)
            mine.append(base[i])
            theirs.append(across)
            blocks.append((z - i) % nz * ny + y)
            for j in range(1, ny):
                moved = permute(base[i], dy=j)
                mine.append(moved)
                theirs.append(permute(moved, dx=1) if i % 2 else permute(across, dy=j))
                blocks.append((z - i) % nz * ny + (y - j) % ny)
        if base[0].shape[1] % 128:
            place = (y - jnp.arange(ny)) % ny

            def merged(group):
                joined = []
                for i in range(nz):
                    stacked = jnp.stack(group[i * ny : (i + 1) * ny])[place]
                    joined.append(jnp.moveaxis(stacked, 0, 1).reshape(stacked.shape[1], -1))
                return joined

            mine, theirs = merged(mine), merged(theirs)
            blocks = [(z - i) % nz for i in range(nz)]
        blocks = jnp.stack(blocks).astype(jnp.int32)

        q_norm = normed(query_latent, query_gain).astype(BF16)
        q_plain = mm(q_norm, w_query_plain).astype(BF16)
        q_raw = mm(q_norm, w_query_rotary).reshape(tok, heads, ROPE)
        qa, qb = q_raw[..., : ROPE // 2], q_raw[..., ROPE // 2 :]
        cos_q, sin_q = cosine[:, None, :], sine[:, None, :]
        q_rot = jnp.concatenate([qa * cos_q - qb * sin_q, qb * cos_q + qa * sin_q], axis=-1)
        q_rot = q_rot.astype(BF16).reshape(tok, heads * ROPE)

        n = len(kv)
        share = tok // n_tp
        own, other = pl.pallas_call(
            functools.partial(attention_kernel, n, half),
            out_shape=(
                jax.ShapeDtypeStruct((nx * share, width), F32),
                jax.ShapeDtypeStruct((nx * share, width), BF16),
            ),
            in_specs=[SMEM] + vmem(5 + n),
            out_specs=tuple(vmem(2)),
            scratch_shapes=[
                pltpu.VMEM((n * half, heads * NOPE), BF16),
                pltpu.VMEM((n * half, heads * VDIM), BF16),
                pltpu.VMEM((ROPE, n * half), BF16),
                pltpu.VMEM((tok, heads * VDIM), BF16),
            ],
            compiler_params=pltpu.CompilerParams(vmem_limit_bytes=56 << 20),
            name="attention",
        )(c[None].astype(jnp.int32), q_plain, q_rot, w_key_plain, w_value, w_output, *kv)
        chip = own + permute(other, dc=1).astype(F32)
        chip = chip.reshape(nx, share, width)
        keep = lax.dynamic_index_in_dim(chip, x, 0, keepdims=False)
        give = lax.dynamic_index_in_dim(chip, (x + 1) % nx, 0, keepdims=False).astype(BF16)
        resid = lax.dynamic_slice_in_dim(resid_in, t_id * share, share, 0)
        mid = resid.astype(F32) + (keep + permute(give, dx=1).astype(F32))
        h_norm = normed(mid, ffn_gain).astype(BF16)

        tokens = [h_norm] + [permute(h_norm, dz=i) for i in range(1, nz)]
        tokens = tokens + [permute(t, dc=1) for t in tokens]
        nb = len(blocks)
        own, other = pl.pallas_call(
            functools.partial(ffn_kernel, len(tokens), nb, fcols),
            out_shape=(
                jax.ShapeDtypeStruct((nz * share, width), F32),
                jax.ShapeDtypeStruct((nz * share, width), BF16),
            ),
            in_specs=[SMEM] + vmem(len(tokens) + 2 * nb),
            out_specs=tuple(vmem(2)),
            scratch_shapes=[pltpu.VMEM((len(tokens) * share, width), BF16)],
            compiler_params=pltpu.CompilerParams(vmem_limit_bytes=56 << 20),
            name="ffn",
        )(blocks, *tokens, *mine, *theirs)
        chip = (own + permute(other, dc=1).astype(F32)).reshape(nz, share, width)
        out = mid + chip[0]
        for i in range(1, nz):
            out = out + permute(chip[i].astype(BF16), dz=-i).astype(F32)
        return out.astype(BF16)

    return shards


def solution(mesh):
    return jax.shard_map(
        make(mesh),
        mesh=mesh,
        in_specs=(
            P("sp", None),
            P("sp", None),
            P("sp", None),
            P("sp", None),
            P(),
            P(),
            P(None, "tp"),
            P(None, "tp"),
            P(None, "tp"),
            P(None, "tp"),
            P("tp", None),
            P(),
            P("sp", "tp"),
            P("sp", "tp"),
            P("tp", "sp"),
        ),
        out_specs=P(("sp", "tp"), None),
        check_vma=False,
    )
```

```python
import functools

import jax
import jax.numpy as jnp
from jax import lax
from jax.experimental import pallas as pl
from jax.experimental.pallas import tpu as pltpu
from jax.sharding import PartitionSpec as P


NOPE = 128
ROPE = 64
VDIM = 128
EPS = 1e-06


F32 = jnp.float32
BF16 = jnp.bfloat16
NT = (((1,), (1,)), ((), ()))
NN = (((1,), (0,)), ((), ()))


def mm(a, b, dims=NN):
    return lax.dot_general(a, b, dims, preferred_element_type=F32)


def normed(values, gain):
    wide = values.astype(F32)
    return wide * lax.rsqrt(jnp.mean(wide * wide, axis=-1, keepdims=True) + EPS) * gain


def attention_kernel(n, half, first, t_ref, qp_ref, qr_ref, wk_ref, wv_ref, *rest):
    if first:
        pieces = rest[:n]
        top_ref, total_ref, acc_ref = rest[n : n + 3]
    else:
        top_in, total_in, acc_in, wo_ref = rest[:4]
        rest = rest[4:]
        pieces = rest[:n]
        own_ref, core_ref, side_ref, cross_ref = rest[n : n + 4]
        out_ref = rest[-1]
        rest = rest[:-1]
    k_ref, v_ref, r_ref = rest[-4:-1]
    attn_ref = rest[-1]
    width = wk_ref.shape[0]
    rows = ROPE * half // width
    for i, piece in enumerate(pieces):
        lat = piece[:half, :]
        at = pl.ds(i * half, half)
        k_ref[at, :] = mm(lat, wk_ref[...]).astype(BF16)
        v_ref[at, :] = mm(lat, wv_ref[...]).astype(BF16)
        for b in range(width // half):
            r_ref[pl.ds(b * rows, rows), at] = piece[half : half + rows, b * half : (b + 1) * half]
    scale = (NOPE + ROPE) ** (-0.5)
    heads = wk_ref.shape[1] // NOPE
    for h in range(heads):
        lane = slice(h * NOPE, (h + 1) * NOPE)
        score = mm(qp_ref[:, lane], k_ref[:, lane], NT)
        score = (score + mm(qr_ref[:, h * ROPE : (h + 1) * ROPE], r_ref[...])) * scale
        top = jnp.max(score, axis=-1, keepdims=True)
        if not first:
            before = top_in[:, h * NOPE : h * NOPE + 1]
            top = jnp.maximum(top, before)
        weight = jnp.exp(score - top)
        total = jnp.sum(weight, axis=-1, keepdims=True)
        mixed = mm(weight.astype(BF16), v_ref[:, lane])
        if first:
            top_ref[:, lane] = jnp.broadcast_to(top, mixed.shape)
            total_ref[:, lane] = jnp.broadcast_to(total, mixed.shape)
            acc_ref[:, lane] = mixed
        else:
            fade = jnp.exp(before - top)
            total = total + fade * total_in[:, h * NOPE : h * NOPE + 1]
            mixed = mixed + fade * acc_in[:, lane]
            attn_ref[:, lane] = (mixed / total).astype(BF16)
    if first:
        return
    out_ref[...] = mm(attn_ref[...], wo_ref[...])
    share = out_ref.shape[0] // 4
    t = t_ref[0]

    def rows(flip):
        return out_ref[pl.ds(pl.multiple_of((t ^ flip) * share, share), share), :]

    own_ref[...] = rows(0)
    core_ref[...] = rows(1).astype(BF16)
    side_ref[...] = rows(2).astype(BF16)
    cross_ref[...] = rows(3).astype(BF16)


def ffn_kernel(n_tok, n_blk, fcols, b_ref, *rest):
    tok = rest[:n_tok]
    blocks = rest[n_tok : n_tok + n_blk]
    own_ref, other_ref, h_ref = rest[n_tok + n_blk :]
    share = tok[0].shape[0]
    for i, t in enumerate(tok):
        h_ref[i * share : (i + 1) * share, :] = t[...]
    width = blocks[0].shape[1]
    count = n_tok * share
    gate = jnp.zeros((count, fcols), F32)
    upper = jnp.zeros((count, fcols), F32)
    for i, w in enumerate(blocks):
        part = h_ref[:, pl.ds(pl.multiple_of(b_ref[i] * width, width), width)]
        gate = gate + mm(part, w[:fcols, :], NT)
        upper = upper + mm(part, w[fcols : 2 * fcols, :], NT)
    hidden = (gate * jax.nn.sigmoid(gate) * upper).astype(BF16)
    mid = count // 2
    for i, w in enumerate(blocks):
        at = pl.ds(pl.multiple_of(b_ref[i] * width, width), width)
        out = mm(hidden, w[2 * fcols :, :])
        own_ref[:, at] = out[:mid]
        other_ref[:, at] = out[mid:].astype(BF16)


def vmem(n):
    return [pl.BlockSpec(memory_space=pltpu.VMEM)] * n


def small(mib):
    return min(mib, 56) << 20


SMEM = pl.BlockSpec(memory_space=pltpu.SMEM)


def make(mesh):
    n_sp, n_tp = mesh.shape["sp"], mesh.shape["tp"]
    nz = 4
    ny = n_sp // nz
    nc = 2
    nx = n_tp // nc

    def permute(value, dz=0, dy=0, dx=0, dc=0):
        pairs = []
        for s in range(n_sp):
            for t in range(n_tp):
                z, y = divmod(s, ny)
                x, c = divmod(t, nc)
                s2 = (z ^ dz) * ny + (y + dy) % ny
                t2 = (x + dx) % nx * nc + (c + dc) % nc
                pairs.append((s * n_tp + t, s2 * n_tp + t2))
        return lax.ppermute(value, ("sp", "tp"), pairs)

    def shards(
        resid_in,
        query_latent,
        kv_latent,
        rotary_key,
        query_gain,
        kv_gain,
        w_query_plain,
        w_query_rotary,
        w_key_plain,
        w_value,
        w_output,
        ffn_gain,
        w_gate,
        w_up,
        w_down,
    ):
        tok, width = resid_in.shape
        kvr = kv_latent.shape[1]
        heads = w_query_plain.shape[1] // NOPE
        s_id = lax.axis_index("sp")
        t_id = lax.axis_index("tp")
        z, y = s_id // ny, s_id % ny
        c = t_id % nc
        position = (s_id * tok + jnp.arange(tok, dtype=jnp.int32)).astype(F32)
        freq = 10000.0 ** (-jnp.arange(0, ROPE, 2, dtype=F32) / ROPE)
        angle = position[:, None] * freq[None, :]
        cosine = jnp.cos(angle)
        sine = jnp.sin(angle)

        half = tok // nc
        lat = normed(lax.dynamic_slice_in_dim(kv_latent, c * half, half, 0), kv_gain).astype(BF16)
        key = lax.dynamic_slice_in_dim(rotary_key, c * half, half, 0).astype(F32)
        cos_k = lax.dynamic_slice_in_dim(cosine, c * half, half, 0)
        sin_k = lax.dynamic_slice_in_dim(sine, c * half, half, 0)
        ka, kb = key[:, : ROPE // 2], key[:, ROPE // 2 :]
        rot = jnp.concatenate([ka * cos_k - kb * sin_k, kb * cos_k + ka * sin_k], axis=1)
        rot = rot.astype(BF16).T
        per = kvr // half
        rows = ROPE // per
        rot = jnp.concatenate([rot[b * rows : (b + 1) * rows] for b in range(per)], axis=1)
        piece = jnp.concatenate([lat, rot], axis=0)
        kv = [piece] + [permute(piece, dz=i) for i in range(1, nz)]
        far = [permute(p, dy=j) for j in range(1, ny) for p in kv]
        near = [permute(p, dc=1) for p in kv]
        cross = [permute(p, dc=1) for p in far]

        fcols = w_gate.shape[1] // nz
        wg = w_gate.T.reshape(nz, fcols, -1)
        wu = w_up.T.reshape(nz, fcols, -1)
        wd = w_down.reshape(nz, fcols, -1)
        packed = jnp.concatenate([wg, wu, wd], axis=1)

        def weights_for(i):
            return lax.dynamic_index_in_dim(packed, z ^ i, 0, keepdims=False)

        weights, blocks = [], []
        for i in range(nz):
            held = permute(weights_for(i), dz=i) if i else weights_for(0)
            weights.append(held)
            blocks.append((z ^ i) * ny + y)
            for j in range(1, ny):
                weights.append(permute(held, dy=j))
                blocks.append((z ^ i) * ny + (y - j) % ny)
        if weights[0].shape[1] % 128:
            place = (y - jnp.arange(ny)) % ny

            def merged(group):
                joined = []
                for i in range(nz):
                    stacked = jnp.stack(group[i * ny : (i + 1) * ny])[place]
                    joined.append(jnp.moveaxis(stacked, 0, 1).reshape(stacked.shape[1], -1))
                return joined

            weights = merged(weights)
            blocks = [z ^ i for i in range(nz)]
        blocks = jnp.stack(blocks).astype(jnp.int32)

        q_norm = normed(query_latent, query_gain).astype(BF16)
        q_plain = mm(q_norm, w_query_plain).astype(BF16)
        q_raw = mm(q_norm, w_query_rotary).reshape(tok, heads, ROPE)
        qa, qb = q_raw[..., : ROPE // 2], q_raw[..., ROPE // 2 :]
        cos_q, sin_q = cosine[:, None, :], sine[:, None, :]
        q_rot = jnp.concatenate([qa * cos_q - qb * sin_q, qb * cos_q + qa * sin_q], axis=-1)
        q_rot = q_rot.astype(BF16).reshape(tok, heads * ROPE)

        share = tok // n_tp
        t32 = t_id[None].astype(jnp.int32)
        wide = heads * NOPE
        near, far = kv + near, far + cross

        def attend(first, pieces, *extra):
            n = len(pieces)
            share = tok // n_tp
            if first:
                shapes = (jax.ShapeDtypeStruct((tok, wide), F32),) * 3
            else:
                shapes = (jax.ShapeDtypeStruct((share, width), F32),)
                shapes = shapes + (jax.ShapeDtypeStruct((share, width), BF16),) * 3
            return pl.pallas_call(
                functools.partial(attention_kernel, n, half, first),
                out_shape=shapes,
                in_specs=[SMEM] + vmem(4 + len(extra) + n),
                out_specs=tuple(vmem(len(shapes))),
                scratch_shapes=[
                    pltpu.VMEM((n * half, wide), BF16),
                    pltpu.VMEM((n * half, heads * VDIM), BF16),
                    pltpu.VMEM((ROPE, n * half), BF16),
                    pltpu.VMEM((tok, heads * VDIM), BF16),
                ]
                + ([] if first else [pltpu.VMEM((tok, width), F32)]),
                compiler_params=pltpu.CompilerParams(vmem_limit_bytes=small(12 + n)),
                name="attention",
            )(t32, q_plain, q_rot, w_key_plain, w_value, *extra, *pieces)

        share = tok // n_tp
        resid = lax.dynamic_slice_in_dim(resid_in, t_id * share, share, 0)
        stats = attend(True, near)
        own, core, side, cross = attend(False, far, *stats, w_output)
        side = permute(side, dx=1)
        cross = permute(cross, dx=1, dc=1)
        core = permute(core, dc=1)
        summed = (own + core.astype(F32)) + (side.astype(F32) + cross.astype(F32))
        mid = resid.astype(F32) + summed
        h_norm = normed(mid, ffn_gain).astype(BF16)

        nb = len(blocks)

        def reduced(i):
            tokens = sides[i][0] + sides[i][1]
            count = len(tokens) * share
            own, other = pl.pallas_call(
                functools.partial(ffn_kernel, len(tokens), nb, fcols),
                out_shape=(
                    jax.ShapeDtypeStruct((count // nc, width), F32),
                    jax.ShapeDtypeStruct((count // nc, width), BF16),
                ),
                in_specs=[SMEM] + vmem(len(tokens) + nb),
                out_specs=tuple(vmem(2)),
                scratch_shapes=[pltpu.VMEM((count, width), BF16)],
                compiler_params=pltpu.CompilerParams(vmem_limit_bytes=small(14)),
                name="ffn",
            )(blocks, *tokens, *weights)
            return own + permute(other, dc=1).astype(F32)

        def halved(chip):
            back = permute(chip[share:].astype(BF16), dx=1)
            return chip[:share] + back.astype(F32)

        opposite = permute(h_norm, dz=3)
        held = [h_norm, permute(h_norm, dz=1), permute(opposite, dz=1), opposite]
        across = [permute(held[0], dx=1)]
        across.append(permute(across[0], dz=1))
        across = across + [permute(held[i], dx=1) for i in range(2, nz)]
        sides = []
        for i in range(nz):
            near = [permute(held[i], dc=1), permute(across[i], dc=1)]
            sides.append(([held[i], across[i]], near))
        chip = reduced(0) + permute(reduced(1).astype(BF16), dz=1).astype(F32)
        out = mid + halved(chip)
        passed = permute(halved(reduced(3)).astype(BF16), dz=1).astype(F32)
        block = (halved(reduced(2)) + passed).astype(BF16)
        out = out + permute(block, dz=2).astype(F32)
        return out.astype(BF16)

    return shards


def solution(mesh):
    return jax.shard_map(
        make(mesh),
        mesh=mesh,
        in_specs=(
            P("sp", None),
            P("sp", None),
            P("sp", None),
            P("sp", None),
            P(),
            P(),
            P(None, "tp"),
            P(None, "tp"),
            P(None, "tp"),
            P(None, "tp"),
            P("tp", None),
            P(),
            P("sp", "tp"),
            P("sp", "tp"),
            P("tp", "sp"),
        ),
        out_specs=P(("sp", "tp"), None),
        check_vma=False,
    )
```

```python
import functools

import jax
import jax.numpy as jnp
from jax import lax
from jax.experimental import pallas as pl
from jax.experimental.pallas import tpu as pltpu
from jax.sharding import PartitionSpec as P


NOPE = 128
ROPE = 64
VDIM = 128
EPS = 1e-06


F32 = jnp.float32
BF16 = jnp.bfloat16
NT = (((1,), (1,)), ((), ()))
NN = (((1,), (0,)), ((), ()))


def mm(a, b, dims=NN):
    return lax.dot_general(a, b, dims, preferred_element_type=F32)


def normed(values, gain):
    wide = values.astype(F32)
    return wide * lax.rsqrt(jnp.mean(wide * wide, axis=-1, keepdims=True) + EPS) * gain


def attention_kernel(n, half, first, t_ref, qp_ref, qr_ref, wk_ref, wv_ref, *rest):
    if first:
        pieces = rest[:n]
        top_ref, total_ref, acc_ref = rest[n : n + 3]
    else:
        top_in, total_in, acc_in, wo_ref = rest[:4]
        rest = rest[4:]
        pieces = rest[:n]
        own_ref, core_ref, side_ref, cross_ref = rest[n : n + 4]
        out_ref = rest[-1]
        rest = rest[:-1]
    k_ref, v_ref, r_ref = rest[-4:-1]
    attn_ref = rest[-1]
    width = wk_ref.shape[0]
    rows = ROPE * half // width
    for i, piece in enumerate(pieces):
        lat = piece[:half, :]
        at = pl.ds(i * half, half)
        k_ref[at, :] = mm(lat, wk_ref[...]).astype(BF16)
        v_ref[at, :] = mm(lat, wv_ref[...]).astype(BF16)
        for b in range(width // half):
            r_ref[pl.ds(b * rows, rows), at] = piece[half : half + rows, b * half : (b + 1) * half]
    scale = (NOPE + ROPE) ** (-0.5)
    heads = wk_ref.shape[1] // NOPE
    for h in range(heads):
        lane = slice(h * NOPE, (h + 1) * NOPE)
        score = mm(qp_ref[:, lane], k_ref[:, lane], NT)
        score = (score + mm(qr_ref[:, h * ROPE : (h + 1) * ROPE], r_ref[...])) * scale
        top = jnp.max(score, axis=-1, keepdims=True)
        if not first:
            before = top_in[:, h * NOPE : h * NOPE + 1]
            top = jnp.maximum(top, before)
        weight = jnp.exp(score - top)
        total = jnp.sum(weight, axis=-1, keepdims=True)
        mixed = mm(weight.astype(BF16), v_ref[:, lane])
        if first:
            top_ref[:, lane] = jnp.broadcast_to(top, mixed.shape)
            total_ref[:, lane] = jnp.broadcast_to(total, mixed.shape)
            acc_ref[:, lane] = mixed
        else:
            fade = jnp.exp(before - top)
            total = total + fade * total_in[:, h * NOPE : h * NOPE + 1]
            mixed = mixed + fade * acc_in[:, lane]
            attn_ref[:, lane] = (mixed / total).astype(BF16)
    if first:
        return
    out_ref[...] = mm(attn_ref[...], wo_ref[...])
    share = out_ref.shape[0] // 4
    t = t_ref[0]

    def rows(flip):
        return out_ref[pl.ds(pl.multiple_of((t ^ flip) * share, share), share), :]

    own_ref[...] = rows(0)
    core_ref[...] = rows(1).astype(BF16)
    side_ref[...] = rows(2).astype(BF16)
    cross_ref[...] = rows(3).astype(BF16)


def ffn_kernel(n_tok, n_blk, fcols, b_ref, *rest):
    tok = rest[:n_tok]
    blocks = rest[n_tok : n_tok + n_blk]
    own_ref, other_ref, h_ref = rest[n_tok + n_blk :]
    share = tok[0].shape[0]
    for i, t in enumerate(tok):
        h_ref[i * share : (i + 1) * share, :] = t[...]
    width = blocks[0].shape[1]
    count = n_tok * share
    gate = jnp.zeros((count, fcols), F32)
    upper = jnp.zeros((count, fcols), F32)
    for i, w in enumerate(blocks):
        part = h_ref[:, pl.ds(pl.multiple_of(b_ref[i] * width, width), width)]
        gate = gate + mm(part, w[:fcols, :], NT)
        upper = upper + mm(part, w[fcols : 2 * fcols, :], NT)
    hidden = (gate * jax.nn.sigmoid(gate) * upper).astype(BF16)
    mid = count // 2
    for i, w in enumerate(blocks):
        at = pl.ds(pl.multiple_of(b_ref[i] * width, width), width)
        out = mm(hidden, w[2 * fcols :, :])
        own_ref[:, at] = out[:mid]
        other_ref[:, at] = out[mid:].astype(BF16)


def vmem(n):
    return [pl.BlockSpec(memory_space=pltpu.VMEM)] * n


def small(mib):
    return min(mib, 56) << 20


SMEM = pl.BlockSpec(memory_space=pltpu.SMEM)


def make(mesh):
    n_sp, n_tp = mesh.shape["sp"], mesh.shape["tp"]
    nz = 4
    ny = n_sp // nz
    nc = 2
    nx = n_tp // nc

    def permute(value, dz=0, dy=0, dx=0, dc=0):
        pairs = []
        for s in range(n_sp):
            for t in range(n_tp):
                z, y = divmod(s, ny)
                x, c = divmod(t, nc)
                s2 = (z ^ dz) * ny + (y + dy) % ny
                t2 = (x + dx) % nx * nc + (c + dc) % nc
                pairs.append((s * n_tp + t, s2 * n_tp + t2))
        return lax.ppermute(value, ("sp", "tp"), pairs)

    def shards(
        resid_in,
        query_latent,
        kv_latent,
        rotary_key,
        query_gain,
        kv_gain,
        w_query_plain,
        w_query_rotary,
        w_key_plain,
        w_value,
        w_output,
        ffn_gain,
        w_gate,
        w_up,
        w_down,
    ):
        tok, width = resid_in.shape
        kvr = kv_latent.shape[1]
        heads = w_query_plain.shape[1] // NOPE
        s_id = lax.axis_index("sp")
        t_id = lax.axis_index("tp")
        z, y = s_id // ny, s_id % ny
        c = t_id % nc
        position = (s_id * tok + jnp.arange(tok, dtype=jnp.int32)).astype(F32)
        freq = 10000.0 ** (-jnp.arange(0, ROPE, 2, dtype=F32) / ROPE)
        angle = position[:, None] * freq[None, :]
        cosine = jnp.cos(angle)
        sine = jnp.sin(angle)

        half = tok // nc
        lat = normed(lax.dynamic_slice_in_dim(kv_latent, c * half, half, 0), kv_gain).astype(BF16)
        key = lax.dynamic_slice_in_dim(rotary_key, c * half, half, 0).astype(F32)
        cos_k = lax.dynamic_slice_in_dim(cosine, c * half, half, 0)
        sin_k = lax.dynamic_slice_in_dim(sine, c * half, half, 0)
        ka, kb = key[:, : ROPE // 2], key[:, ROPE // 2 :]
        rot = jnp.concatenate([ka * cos_k - kb * sin_k, kb * cos_k + ka * sin_k], axis=1)
        rot = rot.astype(BF16).T
        per = kvr // half
        rows = ROPE // per
        rot = jnp.concatenate([rot[b * rows : (b + 1) * rows] for b in range(per)], axis=1)
        piece = jnp.concatenate([lat, rot], axis=0)
        kv = [piece] + [permute(piece, dz=i) for i in range(1, nz)]
        far = [permute(p, dy=j) for j in range(1, ny) for p in kv]
        near = [permute(p, dc=1) for p in kv]
        cross = [permute(p, dc=1) for p in far]

        fcols = w_gate.shape[1] // nz
        wg = w_gate.T.reshape(nz, fcols, -1)
        wu = w_up.T.reshape(nz, fcols, -1)
        wd = w_down.reshape(nz, fcols, -1)
        packed = jnp.concatenate([wg, wu, wd], axis=1)

        def weights_for(i):
            return lax.dynamic_index_in_dim(packed, z ^ i, 0, keepdims=False)

        weights, blocks = [], []
        for i in range(nz):
            held = permute(weights_for(i), dz=i) if i else weights_for(0)
            weights.append(held)
            blocks.append((z ^ i) * ny + y)
            for j in range(1, ny):
                weights.append(permute(held, dy=j))
                blocks.append((z ^ i) * ny + (y - j) % ny)
        if weights[0].shape[1] % 128:
            place = (y - jnp.arange(ny)) % ny

            def merged(group):
                joined = []
                for i in range(nz):
                    stacked = jnp.stack(group[i * ny : (i + 1) * ny])[place]
                    joined.append(jnp.moveaxis(stacked, 0, 1).reshape(stacked.shape[1], -1))
                return joined

            weights = merged(weights)
            blocks = [z ^ i for i in range(nz)]
        blocks = jnp.stack(blocks).astype(jnp.int32)

        q_norm = normed(query_latent, query_gain).astype(BF16)
        q_plain = mm(q_norm, w_query_plain).astype(BF16)
        q_raw = mm(q_norm, w_query_rotary).reshape(tok, heads, ROPE)
        qa, qb = q_raw[..., : ROPE // 2], q_raw[..., ROPE // 2 :]
        cos_q, sin_q = cosine[:, None, :], sine[:, None, :]
        q_rot = jnp.concatenate([qa * cos_q - qb * sin_q, qb * cos_q + qa * sin_q], axis=-1)
        q_rot = q_rot.astype(BF16).reshape(tok, heads * ROPE)

        share = tok // n_tp
        t32 = t_id[None].astype(jnp.int32)
        wide = heads * NOPE
        near, far = kv + near, far + cross

        def attend(first, pieces, *extra):
            n = len(pieces)
            share = tok // n_tp
            if first:
                shapes = (jax.ShapeDtypeStruct((tok, wide), F32),) * 3
            else:
                shapes = (jax.ShapeDtypeStruct((share, width), F32),)
                shapes = shapes + (jax.ShapeDtypeStruct((share, width), BF16),) * 3
            return pl.pallas_call(
                functools.partial(attention_kernel, n, half, first),
                out_shape=shapes,
                in_specs=[SMEM] + vmem(4 + len(extra) + n),
                out_specs=tuple(vmem(len(shapes))),
                scratch_shapes=[
                    pltpu.VMEM((n * half, wide), BF16),
                    pltpu.VMEM((n * half, heads * VDIM), BF16),
                    pltpu.VMEM((ROPE, n * half), BF16),
                    pltpu.VMEM((tok, heads * VDIM), BF16),
                ]
                + ([] if first else [pltpu.VMEM((tok, width), F32)]),
                compiler_params=pltpu.CompilerParams(vmem_limit_bytes=small(12 + n)),
                cost_estimate=pl.CostEstimate(
                    flops=2 * n * half * wide * (2 * kvr + 3 * tok),
                    bytes_accessed=2 * n * half * kvr,
                    transcendentals=n * half * tok * heads,
                ),
                name="attention",
            )(t32, q_plain, q_rot, w_key_plain, w_value, *extra, *pieces)

        share = tok // n_tp
        resid = lax.dynamic_slice_in_dim(resid_in, t_id * share, share, 0)
        stats = attend(True, near)
        own, core, side, cross = attend(False, far, *stats, w_output)
        side = permute(side, dx=1)
        cross = permute(cross, dx=1, dc=1)
        core = permute(core, dc=1)
        summed = (own + core.astype(F32)) + (side.astype(F32) + cross.astype(F32))
        mid = resid.astype(F32) + summed
        h_norm = normed(mid, ffn_gain).astype(BF16)

        nb = len(blocks)

        def reduced(i):
            tokens = sides[i][0] + sides[i][1]
            count = len(tokens) * share
            own, other = pl.pallas_call(
                functools.partial(ffn_kernel, len(tokens), nb, fcols),
                out_shape=(
                    jax.ShapeDtypeStruct((count // nc, width), F32),
                    jax.ShapeDtypeStruct((count // nc, width), BF16),
                ),
                in_specs=[SMEM] + vmem(len(tokens) + nb),
                out_specs=tuple(vmem(2)),
                scratch_shapes=[pltpu.VMEM((count, width), BF16)],
                compiler_params=pltpu.CompilerParams(vmem_limit_bytes=small(14)),
                cost_estimate=pl.CostEstimate(
                    flops=6 * count * width * fcols,
                    bytes_accessed=6 * width * fcols,
                    transcendentals=count * fcols,
                ),
                name="ffn",
            )(blocks, *tokens, *weights)
            return own + permute(other, dc=1).astype(F32)

        def halved(chip):
            back = permute(chip[share:].astype(BF16), dx=1)
            return chip[:share] + back.astype(F32)

        opposite = permute(h_norm, dz=3)
        held = [h_norm, permute(h_norm, dz=1), permute(opposite, dz=1), opposite]
        across = [permute(held[0], dx=1)]
        across.append(permute(across[0], dz=1))
        across = across + [permute(held[i], dx=1) for i in range(2, nz)]
        sides = []
        for i in range(nz):
            near = [permute(held[i], dc=1), permute(across[i], dc=1)]
            sides.append(([held[i], across[i]], near))
        chip = reduced(0) + permute(reduced(1).astype(BF16), dz=1).astype(F32)
        out = mid + halved(chip)
        passed = permute(halved(reduced(3)).astype(BF16), dz=1).astype(F32)
        block = (halved(reduced(2)) + passed).astype(BF16)
        out = out + permute(block, dz=2).astype(F32)
        return out.astype(BF16)

    return shards


def solution(mesh):
    return jax.shard_map(
        make(mesh),
        mesh=mesh,
        in_specs=(
            P("sp", None),
            P("sp", None),
            P("sp", None),
            P("sp", None),
            P(),
            P(),
            P(None, "tp"),
            P(None, "tp"),
            P(None, "tp"),
            P(None, "tp"),
            P("tp", None),
            P(),
            P("sp", "tp"),
            P("sp", "tp"),
            P("tp", "sp"),
        ),
        out_specs=P(("sp", "tp"), None),
        check_vma=False,
    )
```
